128 devices in a mesh: fs: 16 (over z, y), tp: 8 (over x, core).
Axes of the slice: x: 4, y: 4, z: 4, core: 2. Of those that a mesh axis runs over, the one named last changes fastest.
Arguments:
- tokens: bfloat16 [16384, 2048], P('fs', 'tp'), may hold values from -40 to 40
- first_gain: float32 [2048], replicated, may hold values from 0.1 to 1.9
- first_gate: bfloat16 [2048, 6144], P('fs', 'tp'), may hold values from -0.125 to 0.125
- first_upward: bfloat16 [2048, 6144], P('fs', 'tp'), may hold values from -0.125 to 0.125
- first_down: bfloat16 [6144, 2048], P('tp', 'fs'), may hold values from -0.078125 to 0.078125
- mix_gain: float32 [2048], replicated, may hold values from 0.1 to 1.9
- mix_input: bfloat16 [2048, 1024], P('fs', 'tp'), may hold values from -0.125 to 0.125
- pool_weight: bfloat16 [8, 128, 128], replicated, may hold values from -0.5 to 0.5
- pool_scale: float32 [1024], replicated, may hold values from 0.1 to 1.9
- mix_output: bfloat16 [1024, 2048], P('tp', 'fs'), may hold values from -0.1875 to 0.1875
- second_gain: float32 [2048], replicated, may hold values from 0.1 to 1.9
- second_gate: bfloat16 [2048, 6144], P('fs', 'tp'), may hold values from -0.125 to 0.125
- second_upward: bfloat16 [2048, 6144], P('fs', 'tp'), may hold values from -0.125 to 0.125
- second_down: bfloat16 [6144, 2048], P('tp', 'fs'), may hold values from -0.078125 to 0.078125
Outputs:
- layer_out: bfloat16 [16384, 2048], P('fs', 'tp')
The draws below stay inside these ranges and needn't reach their ends.
All inputs are finite; a program needn't handle non-finite values.
Results may differ from the reference program's by a relative error of at most 0.01.
Values may be sent and summed in bfloat16 or wider, within the bound.
A program may use at most 128 MiB of HBM per device.

```python
import math
import jax
import jax.numpy as jnp
from jax import lax

D = 2048
FF = 6144
GROUPS = 8
GROUP_DIM = 128
TOK_DEV = 1024
POOL_WIDTH = 1024
TOKENS = 16384
N_FS = 16
N_TP = 8


def draw_tokens(key, part):
    keys = jax.random.split(jax.random.fold_in(key, 11), 3)
    base = jax.random.normal(keys[0], (TOKENS, D), jnp.float32)
    base = jnp.clip(base, -4.0, 4.0)
    row_scale = jnp.exp(jax.random.uniform(keys[1], (TOKENS, 1), jnp.float32, math.log(0.5), math.log(5.0)))
    col_scale = jnp.exp(jax.random.uniform(keys[2], (1, D), jnp.float32, math.log(0.5), math.log(2.0)))
    return (base * row_scale * col_scale).astype(jnp.bfloat16)


def shard_levels(stream_key, shape, shards, low, high):
    gain, own = 1.0, jax.random.fold_in(stream_key, 6)
    for axis_at, blocks in shards:
        draws = jnp.exp(jax.random.uniform(jax.random.fold_in(own, axis_at), (blocks,), jnp.float32, low / len(shards), high / len(shards)))
        gain = gain * jnp.repeat(draws, shape[axis_at] // blocks).reshape([-1 if axis == axis_at else 1 for axis in range(len(shape))])
    return gain


def normal_values(key, dims, scale, limit, shards=(), kind=jnp.bfloat16):
    values = scale * jax.random.normal(key, dims, jnp.float32)
    if shards:
        values = values * shard_levels(key, dims, shards, -0.22, 0.18)
    return jnp.clip(values, -limit, limit).astype(kind)


def setup_inputs(seed: int = 0) -> dict:
    streams_of = jax.random.split(jax.random.key(seed), 15)
    tokens = draw_tokens(jax.random.fold_in(streams_of[14], 71), 0)
    first_gain = jnp.clip(1.0 + 0.18 * jax.random.normal(streams_of[1], (D,), jnp.float32), 0.1, 1.9)
    first_gate = normal_values(streams_of[2], (D, FF), D ** -0.5, 0.125, ((0, 16), (1, 8)))
    first_upward = normal_values(streams_of[3], (D, FF), D ** -0.5, 0.125, ((0, 16), (1, 8)))
    first_down = normal_values(streams_of[4], (FF, D), FF ** -0.5, 0.078125, ((0, 8), (1, 16)))
    mix_gain = jnp.clip(1.0 + 0.18 * jax.random.normal(streams_of[5], (D,), jnp.float32), 0.1, 1.9)
    mix_input = normal_values(streams_of[6], (D, POOL_WIDTH), D ** -0.5, 0.125, ((0, 16), (1, 8)))
    pool_weight = normal_values(streams_of[7], (GROUPS, GROUP_DIM, GROUP_DIM), GROUP_DIM ** -0.5, 0.5)
    pool_scale = jnp.clip(1.0 + 0.18 * jax.random.normal(streams_of[8], (POOL_WIDTH,), jnp.float32), 0.1, 1.9)
    mix_output = normal_values(streams_of[9], (POOL_WIDTH, D), POOL_WIDTH ** -0.5, 0.1875, ((0, 8), (1, 16)))
    second_gain = jnp.clip(1.0 + 0.18 * jax.random.normal(streams_of[10], (D,), jnp.float32), 0.1, 1.9)
    second_gate = normal_values(streams_of[11], (D, FF), D ** -0.5, 0.125, ((0, 16), (1, 8)))
    second_upward = normal_values(streams_of[12], (D, FF), D ** -0.5, 0.125, ((0, 16), (1, 8)))
    second_down = normal_values(streams_of[13], (FF, D), FF ** -0.5, 0.078125, ((0, 8), (1, 16)))
    return {"tokens": tokens, "first_gain": first_gain, "first_gate": first_gate, "first_upward": first_upward, "first_down": first_down, "mix_gain": mix_gain, "mix_input": mix_input, "pool_weight": pool_weight, "pool_scale": pool_scale, "mix_output": mix_output, "second_gain": second_gain, "second_gate": second_gate, "second_upward": second_upward, "second_down": second_down}


EPSILON = 1e-06
REACH = 15

def normalize(values, weight_gain):
    wide = values.astype(jnp.float32)
    factor = lax.rsqrt(lax.optimization_barrier(jnp.mean(wide * wide, axis=-1, keepdims=True)) + EPSILON)
    return (wide * factor * weight_gain).astype(jnp.bfloat16)

def block_sum(left, right):
    width = left.shape[1] // N_TP
    summed = jnp.zeros((left.shape[0], right.shape[1]), jnp.float32)
    for block in range(N_TP):
        piece = jnp.dot(left[:, block * width:(block + 1) * width], right[block * width:(block + 1) * width], preferred_element_type=jnp.float32)
        summed = summed + lax.optimization_barrier(piece.astype(jnp.bfloat16)).astype(jnp.float32)
    return summed

def feed_forward(values, weight_gain, gate_weight, upward_weight, down_weight):
    normed = normalize(values, weight_gain)
    gated = jnp.dot(normed, gate_weight, preferred_element_type=jnp.float32)
    upward = jnp.dot(normed, upward_weight, preferred_element_type=jnp.float32)
    hidden = (jax.nn.silu(gated) * upward).astype(jnp.bfloat16)
    summed = block_sum(hidden, down_weight)
    return (values.astype(jnp.float32) + 0.5 * summed).astype(jnp.bfloat16)

def pool_mixer(values, mix_gain, mix_input, pool_weight, pool_scale, mix_output):
    normed = normalize(values, mix_gain)
    pool_in = jnp.dot(normed, mix_input, preferred_element_type=jnp.float32).astype(jnp.bfloat16)
    width = pool_in.shape[1]
    sequences = pool_in.reshape(N_FS, TOK_DEV, width).astype(jnp.float32)
    padded = jnp.pad(sequences, ((0, 0), (REACH, 0), (0, 0)))
    windows = jnp.left_shift(2, jnp.arange(GROUPS, dtype=jnp.int32) % 4)
    window_cols = jnp.repeat(windows, GROUP_DIM)[None, None, :]
    summed = jnp.zeros(sequences.shape, jnp.float32)
    for offset in range(REACH + 1):
        shifted = padded[:, REACH - offset:REACH - offset + TOK_DEV]
        summed = summed + jnp.where(offset < window_cols, shifted, 0.0)
    positions = jnp.arange(TOK_DEV, dtype=jnp.int32)
    counts = jnp.minimum(positions[None, :, None] + 1, window_cols).astype(jnp.float32)
    pooled = (summed / counts - sequences).astype(jnp.bfloat16).reshape(TOKENS, GROUPS, GROUP_DIM)
    mapped = jnp.einsum('tgc,gcd->tgd', pooled.astype(jnp.float32), pool_weight.astype(jnp.float32))
    mapped = (mapped.reshape(TOKENS, width) * pool_scale).astype(jnp.bfloat16)
    mixer = block_sum(mapped, mix_output)
    return (values.astype(jnp.float32) + mixer).astype(jnp.bfloat16)

def reference(tokens, first_gain, first_gate, first_upward, first_down, mix_gain, mix_input, pool_weight, pool_scale, mix_output, second_gain, second_gate, second_upward, second_down):
    first_out = feed_forward(tokens, first_gain, first_gate, first_upward, first_down)
    mid_out = pool_mixer(first_out, mix_gain, mix_input, pool_weight, pool_scale, mix_output)
    return feed_forward(mid_out, second_gain, second_gate, second_upward, second_down)
```

```python
import functools

import jax
import jax.numpy as jnp
from jax import lax
from jax.experimental import pallas as pl
from jax.experimental.pallas import tpu as pltpu
from jax.sharding import PartitionSpec as P

EPSILON = 1e-06
CHUNKS = 4
F32 = jnp.float32
BF16 = jnp.bfloat16
VMEM_LIMIT = 66_900_000


class Task:
    def __init__(self, name, waits=(), after=(), work=None, cost=0.05, sends=(), rank=0):
        self.name, self.waits, self.after = name, list(waits), list(after)
        self.work, self.cost, self.sends, self.rank = work, cost, list(sends), rank


def ordered(tasks):
    rate = {"c": 600e3, "l": 1000e3}
    delay = {"c": 1.0, "l": 1.0}
    free, arrive, done, now, out = {}, {}, set(), 0.0, []
    left = list(tasks)
    while left:
        best = None
        for place, task in enumerate(left):
            if any(a not in done for a in task.after) or any(w not in arrive for w in task.waits):
                continue
            ready = max([0.0] + [arrive[w] for w in task.waits])
            key = (max(ready, now), task.rank, ready, place)
            if best is None or key < best[0]:
                best = (key, task)
        assert best is not None, [t.name for t in left]
        task = best[1]
        now = max(now, best[0][0]) + task.cost
        left.remove(task)
        done.add(task.name)
        out.append((now, task))
        for event, link, size, _ in task.sends:
            begin = max(now, free.get(link, 0.0))
            free[link] = begin + size / rate.get(link, 45e3)
            arrive[event] = free[link] + delay.get(link, 2.0)
    return out


def layer_kernel(
    rows_all, width, ring,
    tokens, first_gain, first_gate, first_up, first_down, mix_gain, mix_input, pool_weight, pool_scale, mix_output,
    second_gain, second_gate, second_up, second_down, out,
    gates, ups, downs, mixw, pool_w, feats, hidden, normed, part_send, part_recv, part_own, half_recv, full_recv,
    history, send_sem, recv_sem, local_sem,
):
    fs, tp = lax.axis_index("fs"), lax.axis_index("tp")
    z, y = lax.div(fs, ring), lax.rem(fs, ring)
    x, c = lax.div(tp, 2), lax.rem(tp, 2)
    other = 1 - c

    def step(value, by):
        return lax.rem(value + by + ring, ring)

    devices = {
        "y+": {"fs": z * ring + step(y, 1)}, "y-": {"fs": z * ring + step(y, -1)},
        "z+": {"fs": step(z, 1) * ring + y}, "z-": {"fs": step(z, -1) * ring + y},
        "x+": {"tp": step(x, 1) * 2 + c}, "x-": {"tp": step(x, -1) * 2 + c},
        "c": {"tp": x * 2 + other},
    }
    barrier = pltpu.get_barrier_semaphore()
    for device in devices.values():
        pl.semaphore_signal(barrier, inc=1, device_id=device, device_id_type=pl.DeviceIdType.MESH)
    pl.semaphore_wait(barrier, len(devices))

    count = [0]
    tasks = []

    def size_of(shape):
        total = 2
        for extent in shape:
            total *= extent
        return total

    def remote(event, link, make_src, make_dst, shape):
        slot = count[0]
        count[0] += 1

        def make():
            return pltpu.make_async_remote_copy(
                src_ref=make_src(), dst_ref=make_dst(), send_sem=send_sem.at[slot], recv_sem=recv_sem.at[slot],
                device_id=devices[link], device_id_type=pl.DeviceIdType.MESH,
            )

        return (event, link, size_of(shape), make)

    def same(event, link, make_ref, shape):
        return remote(event, link, make_ref, make_ref, shape)

    locals_made = [0]

    def local(event, make_src, make_dst, shape):
        slot = locals_made[0]
        locals_made[0] += 1

        def make():
            return pltpu.make_async_copy(make_src(), make_dst(), local_sem.at[slot])

        return (event, "l", size_of(shape), make)

    def gather_weights(name, buf, pieces, before):
        rows, cols = buf.shape[2], buf.shape[3]
        half, quarter = rows // 2, rows // 4
        loads = []
        for number, (src, start, length) in enumerate(pieces):
            loads.append(local(
                f"{name}l{number}", lambda src=src: src, lambda start=start, length=length: buf.at[z, y, pl.ds(start, length)],
                (length, cols),
            ))
        tasks.append(Task(f"{name}load", sends=loads, cost=0.01, rank=-2))

        def a_rows(start, length, zz):
            return buf.at[zz, :, pl.ds(start, length)]

        def b_rows(start, length, yy):
            return buf.at[:, yy, pl.ds(start, length)]

        def own(start, length, zz, yy):
            return buf.at[zz, yy, pl.ds(start, length)]

        tasks.append(Task(f"{name}1", waits=[e[0] for e in loads], after=before, sends=[
            same(f"{name}A1+", "y+", lambda: own(0, half, z, y), (half, cols)),
            same(f"{name}A1-", "y-", lambda: own(0, half, z, y), (half, cols)),
            same(f"{name}B1+", "z+", lambda: own(half, half, z, y), (half, cols)),
            same(f"{name}B1-", "z-", lambda: own(half, half, z, y), (half, cols)),
        ]))
        tasks.append(Task(f"{name}2A", waits=[f"{name}A1+", f"{name}A1-"], sends=[
            same(f"{name}A2+", "y+", lambda: own(0, quarter, z, step(y, -1)), (quarter, cols)),
            same(f"{name}A2-", "y-", lambda: own(quarter, quarter, z, step(y, 1)), (quarter, cols)),
        ]))
        tasks.append(Task(f"{name}2B", waits=[f"{name}B1+", f"{name}B1-"], sends=[
            same(f"{name}B2+", "z+", lambda: own(half, quarter, step(z, -1), y), (quarter, cols)),
            same(f"{name}B2-", "z-", lambda: own(half + quarter, quarter, step(z, 1), y), (quarter, cols)),
        ]))
        tasks.append(Task(f"{name}3A", waits=[f"{name}A2+", f"{name}A2-"], after=[f"{name}2A"], sends=[
            same(f"{name}A3+", "z+", lambda: a_rows(0, half, z), (ring, half, cols)),
            same(f"{name}A3-", "z-", lambda: a_rows(0, half, z), (ring, half, cols)),
        ]))
        tasks.append(Task(f"{name}3B", waits=[f"{name}B2+", f"{name}B2-"], after=[f"{name}2B"], sends=[
            same(f"{name}B3+", "y+", lambda: b_rows(half, half, y), (ring, half, cols)),
            same(f"{name}B3-", "y-", lambda: b_rows(half, half, y), (ring, half, cols)),
        ]))
        tasks.append(Task(f"{name}4A", waits=[f"{name}A3+", f"{name}A3-"], sends=[
            same(f"{name}A4+", "z+", lambda: a_rows(0, quarter, step(z, -1)), (ring, quarter, cols)),
            same(f"{name}A4-", "z-", lambda: a_rows(quarter, quarter, step(z, 1)), (ring, quarter, cols)),
        ]))
        tasks.append(Task(f"{name}4B", waits=[f"{name}B3+", f"{name}B3-"], sends=[
            same(f"{name}B4+", "y+", lambda: b_rows(half, quarter, step(y, -1)), (ring, quarter, cols)),
            same(f"{name}B4-", "y-", lambda: b_rows(half + quarter, quarter, step(y, 1)), (ring, quarter, cols)),
        ]))
        tasks.append(Task(f"{name}end", waits=[f"{name}A4+", f"{name}A4-", f"{name}B4+", f"{name}B4-"], rank=0, cost=0.02,
                          after=[f"{name}4A", f"{name}4B"]))

    def block_of(xx, cc):
        return xx * 2 + cc

    def send_own(buf, tag, start, length):
        def own():
            return buf.at[tp, pl.ds(start, length)]
        shape = (length, width)
        return [
            same(f"{tag}p", "x+", own, shape), same(f"{tag}m", "x-", own, shape), same(f"{tag}s0", "c", own, shape),
        ]

    def gather_features(buf, tag, start, length):
        half = length // 2

        def view(xx, begin, extent):
            return buf.at[block_of(xx, c), pl.ds(begin, extent)]

        tasks.append(Task(f"{tag}5", waits=[f"{tag}p", f"{tag}m"], sends=[
            same(f"{tag}fp", "x+", lambda: view(step(x, -1), start, half), (half, width)),
            same(f"{tag}fm", "x-", lambda: view(step(x, 1), start + half, half), (half, width)),
            same(f"{tag}s1", "c", lambda: view(step(x, -1), start, length), (length, width)),
            same(f"{tag}s2", "c", lambda: view(step(x, 1), start, length), (length, width)),
        ]))
        tasks.append(Task(f"{tag}6", waits=[f"{tag}fp", f"{tag}fm"], after=[f"{tag}5"], sends=[
            same(f"{tag}s3", "c", lambda: view(step(x, 2), start, length), (length, width)),
        ]))
        return dict(waits=[f"{tag}s{n}" for n in range(4)], after=[f"{tag}6"])

    def scatter_sums(stage, tag, start, length, before, finish):
        rows = pl.ds(start, length)
        half = length // 2
        low, high = pl.ds(start, half), pl.ds(start + half, half)
        at = stage % 2
        mid = lax.rem
        far, right, left = step(x, 2), step(x, 1), step(x, -1)
        compact = pl.ds(start // 2, half)

        def fold_far():
            total = part_own[at, far, rows].astype(F32) + part_recv[stage, far, rows].astype(F32)
            part_own[at, far, rows] = total.astype(BF16)

        tasks.append(Task(f"{tag}2", waits=[f"{tag}sib"], after=before, work=fold_far, cost=0.2, sends=[
            remote(f"{tag}hp", "x+", lambda: part_own.at[at, far, low], lambda: half_recv.at[stage, 0, compact], (half, width)),
            remote(f"{tag}hm", "x-", lambda: part_own.at[at, far, high], lambda: half_recv.at[stage, 1, compact], (half, width)),
        ]))

        def fold_near():
            for target, extra, plain, number in ((right, low, high, 0), (left, high, low, 1)):
                total = part_own[at, target, extra].astype(F32) + part_recv[stage, target, extra].astype(F32)
                total = total + half_recv[stage, number, compact].astype(F32)
                part_own[at, target, extra] = total.astype(BF16)
                total = part_own[at, target, plain].astype(F32) + part_recv[stage, target, plain].astype(F32)
                part_own[at, target, plain] = total.astype(BF16)

        tasks.append(Task(f"{tag}3", waits=[f"{tag}hp", f"{tag}hm"], after=[f"{tag}2"], work=fold_near, cost=0.3, sends=[
            remote(f"{tag}dp", "x+", lambda: part_own.at[at, right, rows], lambda: full_recv.at[stage, 0, rows], (length, width)),
            remote(f"{tag}dm", "x-", lambda: part_own.at[at, left, rows], lambda: full_recv.at[stage, 1, rows], (length, width)),
        ]))

        def total_rows():
            total = part_own[at, x, rows].astype(F32) + part_recv[stage, x, rows].astype(F32)
            return total + full_recv[stage, 0, rows].astype(F32) + full_recv[stage, 1, rows].astype(F32)

        work, sends = finish(total_rows)
        tasks.append(Task(f"{tag}4", waits=[f"{tag}dp", f"{tag}dm"], after=[f"{tag}3"], work=work, cost=0.3, sends=sends))

    def send_parts(stage, tag, start, length):
        rows = pl.ds(start, length)
        return [remote(
            f"{tag}sib", "c", lambda: part_send.at[stage % 2, :, rows], lambda: part_recv.at[stage, :, rows],
            (ring, length, width),
        )]

    def normalize_rows(stage, gain, start, length):
        sub = 16
        gains = [gain[:, b * width:(b + 1) * width] for b in range(2 * ring)]

        def body(i, carry):
            base = pl.multiple_of(start + i * sub, sub)
            values = [feats[stage, b, pl.ds(base, sub), :].astype(F32) for b in range(2 * ring)]
            squares = functools.reduce(lambda a, b: a + b, [v * v for v in values])
            mean = jnp.sum(squares, axis=-1, keepdims=True) * (1.0 / (2 * ring * width))
            factor = lax.rsqrt(mean + EPSILON)
            for b, v in enumerate(values):
                normed[pl.ds(pl.multiple_of(i * sub, sub), sub), b * width:(b + 1) * width] = (
                    v * factor * gains[b]
                ).astype(BF16)
            return carry

        lax.fori_loop(0, length // sub, body, 0, unroll=2)

    tile = 256

    def hidden_rows(which, stage, gain, start, length):
        def work():
            normalize_rows(stage, gain, start, length)
            depth = 2 * ring * width

            def body(n, carry):
                cols = pl.ds(pl.multiple_of(n * tile, tile), tile)
                gate_w = gates[which, :, :, :, cols].reshape(depth, tile)
                up_w = ups[which, :, :, :, cols].reshape(depth, tile)
                both = jnp.dot(
                    normed[0:length, :], jnp.concatenate([gate_w, up_w], axis=1), preferred_element_type=F32
                )
                gated, upward = both[:, :tile], both[:, tile:]
                value = gated / (1.0 + jnp.exp(-gated)) * upward
                hidden[pl.ds(start, length), cols] = value.astype(BF16)
                return carry

            lax.fori_loop(0, hidden.shape[1] // tile, body, 0)
        return work

    def product_rows(left_value, weight_of, target, slot, side, start, length):
        def body(pair, carry):
            columns = []
            for j in range(2):
                block = block_of(pair * 2 + j, side) * 2
                for k in range(2):
                    index = block + k
                    columns.append(weight_of(lax.div(index, ring), lax.rem(index, ring)))
            value = jnp.dot(left_value(), jnp.concatenate(columns, axis=1), preferred_element_type=F32)
            for j in range(2):
                target[slot, pair * 2 + j, pl.ds(start, length)] = value[:, j * width:(j + 1) * width].astype(BF16)
            return carry

        lax.fori_loop(0, ring // 2, body, 0)

    def down_rows(which, stage, target, side, start, length):
        def work():
            product_rows(
                lambda: hidden[pl.ds(start, length), :], lambda zz, yy: downs[which, zz, yy], target, stage % 2, side,
                start, length,
            )
        return work

    pad = 16

    def pool_rows(start, length):
        def work():
            normalize_rows(1, mix_gain, start, length)
            weight = mixw[:, :, 0:128, :].reshape(2 * ring * width, 128)
            pool_in = jnp.dot(normed[0:length, :], weight, preferred_element_type=F32).astype(BF16).astype(F32)
            if start == 0:
                history[0:pad, :] = jnp.zeros((pad, 128), F32)
            history[pl.ds(pad + start, length), :] = pool_in
            span = history[pl.ds(start, length + pad), :]
            sums = []
            for shift in (1, 2, 4, 8):
                span = span + pltpu.roll(span, shift, 0)
                sums.append(span[pad:, :])
            window = jnp.left_shift(jnp.int32(2), lax.rem(tp, 4))
            total = jnp.where(window == 2, sums[0], jnp.where(window == 4, sums[1], jnp.where(window == 8, sums[2], sums[3])))
            position = start + lax.broadcasted_iota(jnp.int32, (length, 128), 0)
            number = jnp.minimum(position + 1, window).astype(F32)
            pooled = (total / number - pool_in).astype(BF16)
            mapped = jnp.dot(pooled, pool_w[...], preferred_element_type=F32)
            hidden[pl.ds(start, length), 0:128] = (mapped * pool_scale[pl.ds(tp, 1), :]).astype(BF16)
        return work

    def mix_rows(target, side, start, length):
        def work():
            product_rows(
                lambda: hidden[pl.ds(start, length), 0:128], lambda zz, yy: mixw[zz, yy, 128:256, :], target, 1, side,
                start, length,
            )
        return work

    items = [
        ("g1", gates.at[0], [(first_gate, 0, 128)]), ("u1", ups.at[0], [(first_up, 0, 128)]),
        ("d1", downs.at[0], [(first_down, 0, downs.shape[3])]),
        ("mx", mixw, [(mix_input, 0, 128), (mix_output, 128, 128)]),
        ("g2", gates.at[1], [(second_gate, 0, 128)]), ("u2", ups.at[1], [(second_up, 0, 128)]),
        ("d2", downs.at[1], [(second_down, 0, downs.shape[3])]),
    ]
    token_load = local("tok", lambda: tokens, lambda: feats.at[0, tp], (rows_all, width))
    tasks.append(Task("tokload", sends=[token_load], cost=0.01, rank=-3))
    for number, (name, buf, pieces) in enumerate(items):
        before = [f"{items[number - 2][0]}3A", f"{items[number - 2][0]}3B"] if number >= 2 else []
        gather_weights(name, buf, pieces, before)
    tasks.append(Task("poolload", cost=0.01, sends=[local("pw", lambda: pool_weight.at[tp], lambda: pool_w, (128, 128))]))
    tasks.append(Task("tok1", waits=["tok"], sends=send_own(feats.at[0], "t0", 0, rows_all)))
    seen = gather_features(feats.at[0], "t0", 0, rows_all)
    tasks.append(Task("tokend", cost=0.01, **seen))

    length = rows_all // CHUNKS
    for k in range(CHUNKS):
        start = k * length
        rows = pl.ds(start, length)
        tasks.append(Task(f"h1{k}", after=["tokend", "g1end", "u1end"] + ([f"h1{k - 1}"] if k else []),
                          work=hidden_rows(0, 0, first_gain, start, length), cost=2.5, rank=2))
        tasks.append(Task(f"ps0{k}", after=[f"h1{k}", "d1end"], work=down_rows(0, 0, part_send, other, start, length),
                          cost=0.6, rank=1, sends=send_parts(0, f"r0{k}", start, length)))
        tasks.append(Task(f"po0{k}", after=[f"ps0{k}"], work=down_rows(0, 0, part_own, c, start, length), cost=0.6, rank=1))

        def finish_first(total_rows, start=start, rows=rows, k=k):
            def work():
                value = feats[0, tp, rows].astype(F32) + 0.5 * total_rows()
                feats[1, tp, rows] = value.astype(BF16)
            return work, send_own(feats.at[1], f"m{k}", start, length)

        scatter_sums(0, f"r0{k}", start, length, [f"po0{k}"], finish_first)
        seen = gather_features(feats.at[1], f"m{k}", start, length)
        tasks.append(Task(f"pool{k}", waits=seen["waits"] + (["pw"] if k == 0 else []),
                          after=seen["after"] + ["mxend"] + ([f"pool{k - 1}"] if k else []),
                          work=pool_rows(start, length), cost=1.2, rank=1))
        tasks.append(Task(f"ps1{k}", after=[f"pool{k}"], work=mix_rows(part_send, other, start, length),
                          cost=0.3, rank=1, sends=send_parts(1, f"r1{k}", start, length)))
        tasks.append(Task(f"po1{k}", after=[f"ps1{k}"], work=mix_rows(part_own, c, start, length), cost=0.3, rank=1))

        def finish_mixer(total_rows, start=start, rows=rows, k=k):
            def work():
                value = feats[1, tp, rows].astype(F32) + total_rows()
                feats[2, tp, rows] = value.astype(BF16)
            return work, send_own(feats.at[2], f"n{k}", start, length)

        scatter_sums(1, f"r1{k}", start, length, [f"po1{k}"], finish_mixer)
        seen = gather_features(feats.at[2], f"n{k}", start, length)
        reuse = [f"send:r0{k}sib", f"send:r0{k}hp", f"send:r0{k}hm", f"send:r0{k}dp", f"send:r0{k}dm"]
        tasks.append(Task(f"h2{k}", waits=seen["waits"], after=seen["after"] + ["g2end", "u2end", f"ps1{k}", f"po1{k}"],
                          work=hidden_rows(1, 2, second_gain, start, length), cost=2.5, rank=2))
        tasks.append(Task(f"ps2{k}", after=[f"h2{k}", "d2end", f"r0{k}4"], work=down_rows(1, 2, part_send, other, start, length),
                          cost=0.6, rank=1, sends=send_parts(2, f"r2{k}", start, length)))
        tasks[-1].reuse = reuse
        tasks.append(Task(f"po2{k}", after=[f"ps2{k}"], work=down_rows(1, 2, part_own, c, start, length), cost=0.6, rank=1))

        def finish_second(total_rows, rows=rows):
            def work():
                value = feats[2, tp, rows].astype(F32) + 0.5 * total_rows()
                out[rows, :] = value.astype(BF16)
            return work, []

        scatter_sums(2, f"r2{k}", start, length, [f"po2{k}"], finish_second)

    order = ordered(tasks)
    if False:
        for moment, task in order:
            print(f"{moment:8.2f} {task.name}")
    events, sent, waited = {}, {}, set()
    for _, task in order:
        for event in getattr(task, "reuse", []):
            name = event[5:]
            sent.pop(name).wait_send()
        for event in task.waits:
            copy = events[event]
            if isinstance(copy, tuple):
                copy[0].wait()
            else:
                copy.wait_recv()
            waited.add(event)
        if task.work is not None:
            task.work()
        for event, link, _, make in task.sends:
            copy = make()
            copy.start()
            if link == "l":
                events[event] = (copy,)
            else:
                events[event] = copy
                sent[event] = copy
    assert waited == set(events)
    for copy in sent.values():
        copy.wait_send()
    assert count[0] <= send_sem.shape[0] and locals_made[0] <= local_sem.shape[0], (count[0], locals_made[0])


def per_device(
    tokens, first_gain, first_gate, first_up, first_down, mix_gain, mix_input, pool_weight, pool_scale, mix_output,
    second_gain, second_gate, second_up, second_down, *, ring,
):
    rows, width = tokens.shape
    units = first_gate.shape[1]
    model = first_gain.shape[0]
    remote_copies, local_copies = 7 * 16 + 8 + CHUNKS * 31, 10
    flat = lambda gain: gain.reshape(1, model)
    anywhere = pl.BlockSpec(memory_space=pl.ANY)
    inside = pl.BlockSpec(memory_space=pltpu.VMEM)
    scratch = [
        pltpu.VMEM((2, ring, ring, 128, units), BF16),
        pltpu.VMEM((2, ring, ring, 128, units), BF16),
        pltpu.VMEM((2, ring, ring, units, 128), BF16),
        pltpu.VMEM((ring, ring, 256, 128), BF16),
        pltpu.VMEM((128, 128), BF16),
        pltpu.VMEM((3, 2 * ring, rows, width), BF16),
        pltpu.VMEM((rows, units), BF16),
        pltpu.VMEM((rows // CHUNKS, model), BF16),
        pltpu.VMEM((2, ring, rows, width), BF16),
        pltpu.VMEM((3, ring, rows, width), BF16),
        pltpu.VMEM((2, ring, rows, width), BF16),
        pltpu.VMEM((3, 2, rows // 2, width), BF16),
        pltpu.VMEM((3, 2, rows, width), BF16),
        pltpu.VMEM((rows + 16, 128), F32),
        pltpu.SemaphoreType.DMA((remote_copies,)),
        pltpu.SemaphoreType.DMA((remote_copies,)),
        pltpu.SemaphoreType.DMA((local_copies,)),
    ]
    return pl.pallas_call(
        functools.partial(layer_kernel, rows, width, ring),
        out_shape=jax.ShapeDtypeStruct((rows, width), BF16),
        in_specs=[
            anywhere, inside, anywhere, anywhere, anywhere, inside, anywhere, anywhere, inside, anywhere,
            inside, anywhere, anywhere, anywhere,
        ],
        out_specs=inside,
        scratch_shapes=scratch,
        compiler_params=pltpu.CompilerParams(collective_id=0, has_side_effects=True, vmem_limit_bytes=VMEM_LIMIT),
    )(
        tokens, flat(first_gain), first_gate, first_up, first_down, flat(mix_gain), mix_input, pool_weight,
        pool_scale.reshape(-1, 128), mix_output, flat(second_gain), second_gate, second_up, second_down,
    )


def solution(mesh):
    weight, turned = P("fs", "tp"), P("tp", "fs")
    return jax.shard_map(
        functools.partial(per_device, ring=mesh.shape["tp"] // 2),
        mesh=mesh,
        in_specs=(
            P("fs", "tp"), P(), weight, weight, turned, P(), weight, P(), P(), turned, P(), weight, weight, turned,
        ),
        out_specs=P("fs", "tp"),
        check_vma=False,
    )
```

```python
import functools

import jax
import jax.numpy as jnp
from jax import lax
from jax.experimental import pallas as pl
from jax.experimental.pallas import tpu as pltpu
from jax.sharding import PartitionSpec as P

EPSILON = 1e-06
CHUNKS = 4
HALO = 16
F32 = jnp.float32
BF16 = jnp.bfloat16
VMEM_LIMIT = 66_900_000
MESH = pl.DeviceIdType.MESH


class Task:
    def __init__(self, name, waits=(), after=(), work=None, cost=0.05, sends=(), rank=0):
        self.name, self.waits, self.after = name, list(waits), list(after)
        self.work, self.cost, self.sends, self.rank = work, cost, list(sends), rank


def ordered(tasks):
    rate = {"c": 600e3, "l": 1000e3}
    delay = {"c": 1.0, "l": 1.0}
    free, arrive, done, now, out = {}, {}, set(), 0.0, []
    left = list(tasks)
    while left:
        best = None
        for place, task in enumerate(left):
            if any(a not in done for a in task.after) or any(w not in arrive for w in task.waits):
                continue
            ready = max([0.0] + [arrive[w] for w in task.waits])
            key = (max(ready, now), task.rank, ready, place)
            if best is None or key < best[0]:
                best = (key, task)
        assert best is not None, [t.name for t in left]
        task = best[1]
        now = max(now, best[0][0]) + task.cost
        left.remove(task)
        done.add(task.name)
        out.append((now, task))
        for event, link, size, _ in task.sends:
            route = link[:2] if link[0] in "xyz" else link[0]
            begin = max(now, free.get(route, 0.0))
            free[route] = begin + size / rate.get(route, 45e3)
            arrive[event] = free[route] + delay.get(route, 2.0)
    return out


def build(ring, fs, tp, refs):
    (
        tokens, first_gain, first_gate, first_up, first_down, mix_gain, mix_input, pool_weight, pool_scale, mix_output,
        second_gain, second_gate, second_up, second_down, out,
        gates, ups, downs, mixw, feats, middle, hidden, normed, run_normed, first_run, pool_in, halo, mapped_run,
        rows_part, rows_sib, rows_half, rows_full, cols_part, cols_sib, cols_half, cols_full,
        send_sem, recv_sem, local_sem,
    ) = refs
    z, y = lax.div(fs, ring), lax.rem(fs, ring)
    x, c = lax.div(tp, 2), lax.rem(tp, 2)
    other = 1 - c
    blocks = 2 * ring
    rows_all, width = tokens.shape
    model = blocks * width
    length = rows_all // CHUNKS
    run = length // blocks
    lane = 128

    def step(value, by):
        return lax.rem(value + by + ring, ring)

    devices = {
        "y+": {"fs": z * ring + step(y, 1)}, "y-": {"fs": z * ring + step(y, -1)},
        "z+": {"fs": step(z, 1) * ring + y}, "z-": {"fs": step(z, -1) * ring + y},
        "x+": {"tp": step(x, 1) * 2 + c}, "x-": {"tp": step(x, -1) * 2 + c},
        "c": {"tp": x * 2 + other},
        "next": {"tp": lax.rem(tp + 1, blocks)}, "last": {"tp": lax.rem(tp + blocks - 1, blocks)},
    }
    tasks, counts = [], {"r": 0, "l": 0}

    def add(*args, **kwargs):
        tasks.append(Task(*args, **kwargs))

    def size_of(shape):
        total = 2
        for extent in shape:
            total *= extent
        return total

    def remote(event, link, make_src, make_dst, shape):
        slot = counts["r"]
        counts["r"] += 1

        def make():
            return pltpu.make_async_remote_copy(
                src_ref=make_src(), dst_ref=make_dst(), send_sem=send_sem.at[slot], recv_sem=recv_sem.at[slot],
                device_id=devices[link], device_id_type=MESH,
            )

        return (event, "x+" if link == "next" else link, size_of(shape), make)

    def same(event, link, make_ref, shape):
        return remote(event, link, make_ref, make_ref, shape)

    def local(event, make_src, make_dst, shape):
        slot = counts["l"]
        counts["l"] += 1
        return (event, "l", size_of(shape), lambda: pltpu.make_async_copy(make_src(), make_dst(), local_sem.at[slot]))

    def gather_weights(name, buf, pieces, before):
        rows, cols = buf.shape[2], buf.shape[3]
        half, quarter = rows // 2, rows // 4
        loads = [
            local(
                f"{name}l{number}", lambda src=src: src,
                lambda start=start, extent=extent: buf.at[z, y, pl.ds(start, extent)], (extent, cols),
            )
            for number, (src, start, extent) in enumerate(pieces)
        ]
        add(f"{name}load", sends=loads, cost=0.01, rank=-2)

        def a_rows(start, extent, zz):
            return buf.at[zz, :, pl.ds(start, extent)]

        def b_rows(start, extent, yy):
            return buf.at[:, yy, pl.ds(start, extent)]

        def own(start, extent, zz, yy):
            return buf.at[zz, yy, pl.ds(start, extent)]

        add(f"{name}1", waits=[e[0] for e in loads], after=before, sends=[
            same(f"{name}A1+", "y+", lambda: own(0, half, z, y), (half, cols)),
            same(f"{name}A1-", "y-", lambda: own(0, half, z, y), (half, cols)),
            same(f"{name}B1+", "z+", lambda: own(half, half, z, y), (half, cols)),
            same(f"{name}B1-", "z-", lambda: own(half, half, z, y), (half, cols)),
        ])
        add(f"{name}2A", waits=[f"{name}A1+", f"{name}A1-"], sends=[
            same(f"{name}A2+", "y+", lambda: own(0, quarter, z, step(y, -1)), (quarter, cols)),
            same(f"{name}A2-", "y-", lambda: own(quarter, quarter, z, step(y, 1)), (quarter, cols)),
        ])
        add(f"{name}2B", waits=[f"{name}B1+", f"{name}B1-"], sends=[
            same(f"{name}B2+", "z+", lambda: own(half, quarter, step(z, -1), y), (quarter, cols)),
            same(f"{name}B2-", "z-", lambda: own(half + quarter, quarter, step(z, 1), y), (quarter, cols)),
        ])
        add(f"{name}3A", waits=[f"{name}A2+", f"{name}A2-"], after=[f"{name}2A"], sends=[
            same(f"{name}A3+", "z+", lambda: a_rows(0, half, z), (ring, half, cols)),
            same(f"{name}A3-", "z-", lambda: a_rows(0, half, z), (ring, half, cols)),
        ])
        add(f"{name}3B", waits=[f"{name}B2+", f"{name}B2-"], after=[f"{name}2B"], sends=[
            same(f"{name}B3+", "y+", lambda: b_rows(half, half, y), (ring, half, cols)),
            same(f"{name}B3-", "y-", lambda: b_rows(half, half, y), (ring, half, cols)),
        ])
        add(f"{name}4A", waits=[f"{name}A3+", f"{name}A3-"], sends=[
            same(f"{name}A4+", "z+", lambda: a_rows(0, quarter, step(z, -1)), (ring, quarter, cols)),
            same(f"{name}A4-", "z-", lambda: a_rows(quarter, quarter, step(z, 1)), (ring, quarter, cols)),
        ])
        add(f"{name}4B", waits=[f"{name}B3+", f"{name}B3-"], sends=[
            same(f"{name}B4+", "y+", lambda: b_rows(half, quarter, step(y, -1)), (ring, quarter, cols)),
            same(f"{name}B4-", "y-", lambda: b_rows(half + quarter, quarter, step(y, 1)), (ring, quarter, cols)),
        ])
        add(f"{name}endA", waits=[f"{name}A4+", f"{name}A4-"], cost=0.02, after=[f"{name}4A"])
        add(f"{name}endB", waits=[f"{name}B4+", f"{name}B4-"], cost=0.02, after=[f"{name}4B"])

    def ends(*names):
        return [f"{name}end{half}" for name in names for half in "AB"]

    def block_of(xx, cc):
        return xx * 2 + cc

    def send_own(tag, view, size):
        def own():
            return view(tp, 2)
        return [
            same(f"{tag}p", "x+", own, (size,)), same(f"{tag}m", "x-", own, (size,)), same(f"{tag}s0", "c", own, (size,)),
        ]

    def gather_blocks(tag, view, size):
        def at(by, part):
            return view(block_of(step(x, by), c), part)

        add(f"{tag}5", waits=[f"{tag}p", f"{tag}m"], sends=[
            same(f"{tag}fp", "x+", lambda: at(-1, 0), (size // 2,)),
            same(f"{tag}fm", "x-", lambda: at(1, 1), (size // 2,)),
            same(f"{tag}s1", "c", lambda: at(-1, 2), (size,)),
            same(f"{tag}s2", "c", lambda: at(1, 2), (size,)),
        ])
        add(f"{tag}6", waits=[f"{tag}fp", f"{tag}fm"], after=[f"{tag}5"], sends=[
            same(f"{tag}s3", "c", lambda: at(2, 2), (size,)),
        ])
        return dict(waits=[f"{tag}s{n}" for n in range(4)], after=[f"{tag}6"])

    def scatter_sums(tag, bufs, start, extent, before, finish):
        part, sib, half_recv, full_recv = bufs
        cols = part.shape[3]
        rows, half = pl.ds(start, extent), extent // 2
        low, high, compact = pl.ds(start, half), pl.ds(start + half, half), pl.ds(start // 2, half)
        far, right, left = step(x, 2), step(x, 1), step(x, -1)

        def pair(target, which):
            return part[target, c, which].astype(F32) + sib[target, which].astype(F32)

        def fold_far():
            part[far, c, rows] = pair(far, rows).astype(BF16)

        add(f"{tag}2", waits=[f"{tag}sib"], after=before, work=fold_far, cost=0.2, sends=[
            remote(f"{tag}hp", "x+", lambda: part.at[far, c, low], lambda: half_recv.at[0, compact], (half, cols)),
            remote(f"{tag}hm", "x-", lambda: part.at[far, c, high], lambda: half_recv.at[1, compact], (half, cols)),
        ])

        def fold_near():
            for target, extra, plain, number in ((right, low, high, 0), (left, high, low, 1)):
                part[target, c, extra] = (pair(target, extra) + half_recv[number, compact].astype(F32)).astype(BF16)
                part[target, c, plain] = pair(target, plain).astype(BF16)

        add(f"{tag}3", waits=[f"{tag}hp", f"{tag}hm"], after=[f"{tag}2"], work=fold_near, cost=0.3, sends=[
            remote(f"{tag}dp", "x+", lambda: part.at[right, c, rows], lambda: full_recv.at[0, rows], (extent, cols)),
            remote(f"{tag}dm", "x-", lambda: part.at[left, c, rows], lambda: full_recv.at[1, rows], (extent, cols)),
        ])

        def total(span):
            return (
                part[x, c, rows, span].astype(F32) + sib[x, rows, span].astype(F32)
                + full_recv[0, rows, span].astype(F32) + full_recv[1, rows, span].astype(F32)
            )

        work, sends, cost = finish(total)
        add(f"{tag}4", waits=[f"{tag}dp", f"{tag}dm"], after=[f"{tag}3"], work=work, cost=cost, sends=sends)

    def send_parts(tag, bufs, start, extent):
        part, sib = bufs[:2]
        rows = pl.ds(start, extent)
        return [remote(
            f"{tag}sib", "c", lambda: part.at[:, other, rows], lambda: sib.at[:, rows], (ring, extent, part.shape[3]),
        )]

    sub = 16

    def scaled(values, gains):
        squares = functools.reduce(lambda a, b: a + b, [v * v for v in values])
        mean = jnp.sum(squares, axis=-1, keepdims=True) * (1.0 / model)
        factor = lax.rsqrt(mean + EPSILON)
        return [(v * factor * g).astype(BF16) for v, g in zip(values, gains)]

    def normalize_rows(read, gain, start):
        def body(i, carry):
            base = pl.multiple_of(start + i * sub, sub)
            gains = [gain[:, b * width:(b + 1) * width] for b in range(blocks)]
            for b, v in enumerate(scaled([read(b, pl.ds(base, sub)).astype(F32) for b in range(blocks)], gains)):
                normed[pl.ds(base, sub), b * width:(b + 1) * width] = v
            return carry

        lax.fori_loop(0, length // sub, body, 0, unroll=2)

    tile = 256

    def hidden_rows(which, start):
        def work():
            def body(n, carry):
                cols = pl.ds(pl.multiple_of(n * tile, tile), tile)
                gate_w = gates[which, :, :, :, cols].reshape(model, tile)
                up_w = ups[which, :, :, :, cols].reshape(model, tile)
                both = jnp.dot(
                    normed[pl.ds(start, length), :], jnp.concatenate([gate_w, up_w], axis=1),
                    preferred_element_type=F32,
                )
                gated, upward = both[:, :tile], both[:, tile:]
                value = gated / (1.0 + jnp.exp(-gated)) * upward
                hidden[pl.ds(start, length), cols] = value.astype(BF16)
                return carry

            lax.fori_loop(0, hidden.shape[1] // tile, body, 0)
        return work

    def down_rows(which, start, store):
        def work():
            def body(n, carry):
                columns = [downs[which, n, i] for i in range(ring)]
                value = jnp.dot(
                    hidden[pl.ds(start, length), :], jnp.concatenate(columns, axis=1), preferred_element_type=F32
                )
                store(n, value.astype(BF16))
                return carry

            lax.fori_loop(0, ring, body, 0)
        return work

    wide = ring * lane

    def first_finish(k):
        start = k * length

        def finish(total):
            def work():
                place = pl.ds(pl.multiple_of(start + tp * run, run), run)
                for b in range(blocks):
                    span = slice(b * width, (b + 1) * width)
                    value = feats[b, place, :].astype(F32) + 0.5 * total(span)
                    first_run[k * run:(k + 1) * run, span] = value.astype(BF16)
            return work, [], 0.4
        return finish

    def pool_in_rows(k):
        def work():
            gains = [mix_gain[:, b * width:(b + 1) * width] for b in range(blocks)]
            for base in range(0, run, sub):
                rows = pl.ds(k * run + base, sub)
                spans = [slice(b * width, (b + 1) * width) for b in range(blocks)]
                for span, v in zip(spans, scaled([first_run[rows, span].astype(F32) for span in spans], gains)):
                    run_normed[base:base + sub, span] = v

            def body(n, carry):
                columns = [mixw[n * ring + i, :, :, 0:lane, :].reshape(model, lane) for i in range(ring)]
                value = jnp.dot(run_normed[...], jnp.concatenate(columns, axis=1), preferred_element_type=F32)
                pool_in[k, :, pl.ds(pl.multiple_of(n * wide, wide), wide)] = value.astype(BF16)
                return carry

            lax.fori_loop(0, blocks // ring, body, 0)
            if k == 0:
                halo[0] = jnp.zeros(halo.shape[1:], BF16)
        return work

    def mixer_rows(k):
        start = k * length

        def work():
            position = start + tp * run + lax.broadcasted_iota(jnp.int32, (run, lane), 0)
            slot = k + jnp.minimum(tp, 1)
            for b in range(blocks):
                span = slice(b * lane, (b + 1) * lane)
                window = 2 << (b % 4)
                current = pool_in[k, :, span].astype(F32)
                total = jnp.concatenate([halo[slot, :, span].astype(F32), current], axis=0)
                shift = 1
                while shift < window:
                    total = total + pltpu.roll(total, shift, 0)
                    shift *= 2
                number = jnp.minimum(position + 1, window).astype(F32)
                pooled = (total[HALO:, :] / number - current).astype(BF16)
                mapped = jnp.dot(pooled, pool_weight[b], preferred_element_type=F32)
                mapped_run[:, span] = (mapped * pool_scale[b:b + 1, :]).astype(BF16)
            place = pl.ds(pl.multiple_of(start + tp * run, run), run)

            def body(n, carry):
                columns = [mixw[:, n, i, lane:2 * lane, :].reshape(blocks * lane, lane) for i in range(ring)]
                value = jnp.dot(mapped_run[...], jnp.concatenate(columns, axis=1), preferred_element_type=F32)
                cols = pl.ds(pl.multiple_of(n * wide, wide), wide)
                value = first_run[k * run:(k + 1) * run, cols].astype(F32) + value
                middle[place, cols] = value.astype(BF16)
                return carry

            lax.fori_loop(0, ring, body, 0)
        return work

    units = downs.shape[3]
    items = [
        ("g1", gates.at[0], [(first_gate, 0, lane)]), ("u1", ups.at[0], [(first_up, 0, lane)]),
        ("mx", mixw.at[tp], [(mix_input, 0, lane), (mix_output, lane, lane)]),
        ("d1", downs.at[0], [(first_down, 0, units)]),
        ("g2", gates.at[1], [(second_gate, 0, lane)]), ("u2", ups.at[1], [(second_up, 0, lane)]),
        ("d2", downs.at[1], [(second_down, 0, units)]),
    ]
    token_load = local("tok", lambda: tokens, lambda: feats.at[0 + tp], (rows_all, width))
    add("tokload", sends=[token_load], cost=0.01, rank=-3)
    for number, (name, buf, pieces) in enumerate(items):
        before = [f"{items[number - 2][0]}3A", f"{items[number - 2][0]}3B"] if number >= 2 else []
        gather_weights(name, buf, pieces, before)

    def token_view(block, part):
        half = rows_all // 2
        return feats.at[block, pl.ds(*((0, half), (half, half), (0, rows_all))[part])]

    add("tok1", waits=["tok"], sends=send_own("t", token_view, rows_all * width))
    add("tokend", cost=0.01, **gather_blocks("t", token_view, rows_all * width))
    for tag, begin, half_name in (("xi", 0, "A"), ("xo", lane, "B")):
        def mix_view(block, part, begin=begin):
            half = ring // 2
            return mixw.at[block, pl.ds(*((0, half), (half, half), (0, ring))[part]), :, pl.ds(begin, lane)]

        size = ring * ring * lane * lane
        add(f"{tag}1", after=[f"mxend{half_name}"], sends=send_own(tag, mix_view, size))
        add(f"{tag}end", cost=0.01, **gather_blocks(tag, mix_view, size))

    by_rows = (rows_part, rows_sib, rows_half, rows_full)
    by_cols = (cols_part, cols_sib, cols_half, cols_full)
    for k in range(CHUNKS):
        start = k * length
        rows = pl.ds(start, length)
        before = [f"m{k - 1}"] if k else []
        add(f"n1{k}", after=["tokend"], cost=0.8, rank=3,
            work=functools.partial(normalize_rows, lambda b, place: feats[b, place, :], first_gain, start))
        add(f"h1{k}", after=[f"n1{k}"] + ends("g1", "u1"), work=hidden_rows(0, start), cost=2.0, rank=2)

        def store_rows(n, value, k=k):
            cols = pl.ds(pl.multiple_of(n * wide, wide), wide)
            for b in range(blocks):
                rows_part[b // 2, b % 2, k * run:(k + 1) * run, cols] = value[b * run:(b + 1) * run, :]

        add(f"p1{k}", after=[f"h1{k}"] + ends("d1"), work=down_rows(0, start, store_rows), cost=1.1, rank=1,
            sends=send_parts(f"r{k}", by_rows, k * run, run))
        scatter_sums(f"r{k}", by_rows, k * run, run, [f"p1{k}"], first_finish(k))
        add(f"i{k}", after=[f"r{k}4", "xiend"], work=pool_in_rows(k), cost=1.5, rank=1, sends=[remote(
            f"halo{k}", "next", lambda k=k: pool_in.at[k, pl.ds(run - HALO, HALO)], lambda k=k: halo.at[k + 1],
            (HALO, blocks * lane),
        )])

        def run_view(block, part, start=start):
            half = run // 2
            begin, extent = ((0, half), (half, half), (0, run))[part]
            return middle.at[pl.ds(pl.multiple_of(start + block * run + begin, half), extent)]

        add(f"m{k}", waits=[f"halo{k}"], after=[f"i{k}", "xoend"] + before, work=mixer_rows(k), cost=1.8, rank=1,
            sends=send_own(f"a{k}", run_view, run * model))
        seen = gather_blocks(f"a{k}", run_view, run * model)
        add(f"n2{k}", waits=seen["waits"], after=seen["after"] + [f"h1{k}"], cost=0.8, rank=2,
            work=functools.partial(
                normalize_rows, lambda b, place: middle[place, b * width:(b + 1) * width], second_gain, start))
        add(f"h2{k}", after=[f"n2{k}", f"p1{k}"] + ends("g2", "u2"), work=hidden_rows(1, start), cost=2.0, rank=2)

        def store_cols(n, value, rows=rows):
            for b in range(2):
                cols_part[n, b, rows] = value[:, b * width:(b + 1) * width]

        add(f"p2{k}", after=[f"h2{k}"] + ends("d2"), work=down_rows(1, start, store_cols), cost=1.1, rank=1,
            sends=send_parts(f"q{k}", by_cols, start, length))

        def last_finish(total, rows=rows):
            def work():
                cols = pl.ds(pl.multiple_of(tp * width, width), width)
                value = middle[rows, cols].astype(F32) + 0.5 * total(slice(None))
                out[rows, :] = value.astype(BF16)
            return work, [], 0.3

        scatter_sums(f"q{k}", by_cols, start, length, [f"p2{k}"], last_finish)
    return tasks, devices, counts


def layer_kernel(ring, *refs):
    fs, tp = lax.axis_index("fs"), lax.axis_index("tp")
    tasks, devices, counts = build(ring, fs, tp, refs)
    send_sem, recv_sem, local_sem = refs[-3:]
    assert counts["r"] == send_sem.shape[0] and counts["l"] == local_sem.shape[0], counts
    barrier = pltpu.get_barrier_semaphore()
    for device in devices.values():
        pl.semaphore_signal(barrier, inc=1, device_id=device, device_id_type=MESH)
    pl.semaphore_wait(barrier, len(devices))
    events, sent, waited = {}, [], set()
    for _, task in ordered(tasks):
        for event in task.waits:
            link, copy = events[event]
            copy.wait() if link == "l" else copy.wait_recv()
            waited.add(event)
        if task.work is not None:
            task.work()
        for event, link, _, make in task.sends:
            copy = make()
            copy.start()
            events[event] = (link, copy)
            if link != "l":
                sent.append(copy)
    assert waited == set(events)
    for copy in sent:
        copy.wait_send()


def scratch_of(ring, rows, width, units):
    blocks, run, lane = 2 * ring, rows // CHUNKS // (2 * ring), 128
    model, runs = blocks * width, rows // (2 * ring)
    remote_copies, local_copies = 7 * 16 + 8 + 16 + CHUNKS * 19, 9
    return [
        pltpu.VMEM((2, ring, ring, lane, units), BF16),
        pltpu.VMEM((2, ring, ring, lane, units), BF16),
        pltpu.VMEM((2, ring, ring, units, lane), BF16),
        pltpu.VMEM((blocks, ring, ring, 2 * lane, lane), BF16),
        pltpu.VMEM((blocks, rows, width), BF16),
        pltpu.VMEM((rows, model), BF16),
        pltpu.VMEM((rows, units), BF16),
        pltpu.VMEM((rows, model), BF16),
        pltpu.VMEM((run, model), BF16),
        pltpu.VMEM((runs, model), BF16),
        pltpu.VMEM((CHUNKS, run, blocks * lane), BF16),
        pltpu.VMEM((CHUNKS + 1, HALO, blocks * lane), BF16),
        pltpu.VMEM((run, blocks * lane), BF16),
        pltpu.VMEM((ring, 2, runs, model), BF16),
        pltpu.VMEM((ring, runs, model), BF16),
        pltpu.VMEM((2, runs // 2, model), BF16),
        pltpu.VMEM((2, runs, model), BF16),
        pltpu.VMEM((ring, 2, rows, width), BF16),
        pltpu.VMEM((ring, rows, width), BF16),
        pltpu.VMEM((2, rows // 2, width), BF16),
        pltpu.VMEM((2, rows, width), BF16),
        pltpu.SemaphoreType.DMA((remote_copies,)),
        pltpu.SemaphoreType.DMA((remote_copies,)),
        pltpu.SemaphoreType.DMA((local_copies,)),
    ]


def per_device(
    tokens, first_gain, first_gate, first_up, first_down, mix_gain, mix_input, pool_weight, pool_scale, mix_output,
    second_gain, second_gate, second_up, second_down, *, ring,
):
    rows, width = tokens.shape
    anywhere = pl.BlockSpec(memory_space=pl.ANY)
    inside = pl.BlockSpec(memory_space=pltpu.VMEM)
    return pl.pallas_call(
        functools.partial(layer_kernel, ring),
        out_shape=jax.ShapeDtypeStruct((rows, width), BF16),
        in_specs=[
            anywhere, inside, anywhere, anywhere, anywhere, inside, anywhere, inside, inside, anywhere,
            inside, anywhere, anywhere, anywhere,
        ],
        out_specs=inside,
        scratch_shapes=scratch_of(ring, rows, width, first_gate.shape[1]),
        compiler_params=pltpu.CompilerParams(collective_id=0, has_side_effects=True, vmem_limit_bytes=VMEM_LIMIT),
    )(
        tokens, first_gain.reshape(1, -1), first_gate, first_up, first_down, mix_gain.reshape(1, -1), mix_input,
        pool_weight, pool_scale.reshape(-1, 128), mix_output, second_gain.reshape(1, -1), second_gate, second_up,
        second_down,
    )


def solution(mesh):
    weight, turned = P("fs", "tp"), P("tp", "fs")
    return jax.shard_map(
        functools.partial(per_device, ring=mesh.shape["tp"] // 2),
        mesh=mesh,
        in_specs=(
            P("fs", "tp"), P(), weight, weight, turned, P(), weight, P(), P(), turned, P(), weight, weight, turned,
        ),
        out_specs=P("fs", "tp"),
        check_vma=False,
    )
```

```python
import functools

import jax
import jax.numpy as jnp
from jax import lax
from jax.experimental import pallas as pl
from jax.experimental.pallas import tpu as pltpu
from jax.sharding import PartitionSpec as P

EPSILON = 1e-06
CHUNKS = 4
HALO = 16
F32 = jnp.float32
BF16 = jnp.bfloat16
FINE = ('g1', 'mx', 'u1', 'u2')
SEMAPHORES = 205
MEASURES = (22, 23)
VMEM_LIMIT = 64_000_000
MESH = pl.DeviceIdType.MESH


ORDER = (
    "d1load", "u2load", "smallload", "g1load", "g2load", "u1load", "mxload", "tokload", "d2load", "mxload/1",
    "entered", "mx1", "mx1/4", "u11", "tok1", "g11", "mx1/1", "u11/1", "g11/2", "u11/4", "mx1/5", "smallload/3",
    "g11/5", "mx1/7", "mx1/2", "g11/1", "g11/4", "mx1/3", "tok1/1", "mx2A", "mx2B", "mx2A/1", "u11/3", "u11/6",
    "mx1/6", "u12A", "u11/5", "mx2B/4", "mx2B/3", "mx2A/3", "tok1/2", "mx2B/5", "u11/7", "smallload/1", "d1pair",
    "u12A/1", "mx2B/1", "u12A/3", "g12A", "g11/7", "mx3A", "mx2A/2", "mx2A/5", "mx3A/1", "g11/6", "g11/3", "mx2A/4",
    "g12B", "mx4Bo", "u12B", "mx4Bo/1", "smallload/4", "g12A/3", "d1ready", "g12B/5", "u12B/5", "d1a1", "mx2B/2",
    "d1b1", "d1a1/1", "mx3B", "u12A/2", "g12B/4", "mx4Af", "d1b1/1", "mx4Ao", "mx4An", "mx4Af/1", "mx4Ao/1",
    "mx4An/3", "mx3B/1", "t5", "mx4An/1", "g12A/1", "mx4An/2", "t5/1", "u12B/1", "u12A/5", "u12B/4", "g12A/5",
    "g12A/2", "g14Ao", "u12B/3", "t5/2", "d1a1/2", "mx4Bn", "u12A/4", "g12B/2", "g12B/1", "mx4Bn/1", "smallload/2",
    "d1b1/3", "mx4A", "u12B/2", "mxendA", "d1b2A", "xi1", "mx4Bn/3", "g14Ao/1", "xi1/1", "u13B", "g12B/3", "u13B/1",
    "u11/2", "mx4Bf", "mx4Bf/1", "mx4Bn/2", "g13A", "g13A/1", "d1b1/2", "u13A", "t6", "g13B", "u14An", "u14Bn",
    "u14Bn/2", "mx4B", "g13B/1", "u14Bn/3", "xi1/2", "t5/3", "g14Bn", "d1a1/3", "g14Bn/3", "u14Bf", "u14An/3",
    "g12A/4", "u14Bf/1", "u13A/1", "mxendB", "d1b2A/1", "smallend", "xo1", "u14Bo", "u14An/2", "d1a2A", "tokend",
    "g14Bn/1", "g14Bn/2", "d1b2B", "u14Ao", "xo1/1", "u14Ao/1", "u14Bo/1", "n11", "g14Bo", "d1a2B", "u14An/1",
    "d1b2B/1", "n10", "g14Af", "d1a2A/1", "g14Bf", "n12", "u14Bn/1", "d1a2B/1", "g14B", "g14An", "g14Bo/1", "g14An/1",
    "g14An/3", "u14Af", "u14B", "g14An/2", "d1b3B", "u14A", "g14Bf/1", "g14Af/1", "u14Af/1", "d1b3A", "xi5", "g14A",
    "n13", "d1b3B/1", "d1a3A", "d1b3A/1", "d1a3B", "d1a3B/1", "d2pair", "u1endA", "g1endB", "g1endA", "d1a3A/1",
    "xi5/1", "u1endB", "xi5/2", "h10.0", "h10.1", "h12.0", "d1b4B", "xo5", "h11.0", "xo5/1", "h12.1", "xi5/3",
    "d1b4A", "d1b4A/1", "d1b4B/1", "h10", "h12", "h11.1", "d1a4B", "h11", "d1a4B/1", "d1a4A", "d1a4A/1", "u21",
    "u21/1", "u21/5", "u21/4", "g21", "h13.0", "xi6", "h13.1", "g21/1", "d1bendA", "g21/3", "d1bendB", "g21/2",
    "p10b", "p11b", "u21/7", "p12b", "d2ready", "d1aendB", "r0b2", "r0b2/1", "d1aendA", "p10a", "d2a1", "d2a1/2",
    "r1b2", "d2a1/3", "d2a1/1", "d2b1", "r1b2/1", "xo5/3", "r2b2", "p11a", "u22B", "r0a2", "r0a2/1", "u22B/5",
    "xiend", "u22B/1", "u22A", "r0b3", "r2b2/1", "u22A/4", "u22A/5", "u22A/1", "u22B/4", "h13", "u22A/2", "r0b3/1",
    "g22A", "r1a2", "xo5/2", "g22A/1", "r1a2/1", "u22A/3", "r1b3", "g22B", "xo1/2", "g22B/1", "p13b", "u21/3", "p12a",
    "u21/2", "r0a3", "u21/6", "r2b3", "xo6", "r0a3/1", "p13a", "u22B/3", "r2a2", "r1b3/1", "r1a3", "r2a2/1", "r1a3/1",
    "u23B", "u24An", "u23A", "r0a4", "r3b2", "u23A/1", "r3a2", "r3b2/1", "r0b4", "u23B/1", "g23A", "r3a2/1", "u22B/2",
    "g23A/1", "d2b1/2", "u24An/2", "g23B", "d2a2A", "i0", "r2b3/1", "g23B/1", "r2a3", "r1b4", "r1a4", "r2a3/1", "i1",
    "u24Ao", "r3a3", "r3b3", "d2a2B", "d2a2B/1", "u24Bo", "r3b3/1", "xoend", "r3a3/1", "d2b1/1", "b0", "r2b4", "m0",
    "r2a4", "u24Bn", "i2", "u24Af", "b1", "u24Bf", "u24Bf/1", "d2b1/3", "m0/1", "m1", "m1/2", "r3b4", "r3a4",
    "u24An/3", "u24Bn/1", "m0/2", "u24Bn/2", "i3", "m1/1", "d2a2A/1", "u24An/1", "u24Ao/1", "u24Af/1", "u24Bo/1",
    "u24Bn/3", "g24B", "g24A", "a05", "g24A/1", "a05/1", "b2", "m2", "g24B/1", "m2/1", "d2a3B", "u24A", "d2a3A",
    "a15", "d2b2B", "a05/2", "u24B", "b3", "d2b2A", "d2a3B/1", "a06", "d2a3A/1", "a15/3", "a15/1", "a05/3", "m3",
    "m2/2", "d2b2B/1", "m3/1", "u2endB", "a25", "a25/3", "a15/2", "m3/2", "n20", "d2b2A/1", "g2endB", "a16", "u2endA",
    "a25/1", "a25/2", "g2endA", "h20.0", "h20.1", "h20", "n21", "h21.0", "a35", "d2a4B", "d2a4B/1", "d2a4A",
    "d2a4A/1", "a26", "h21.1", "d2b3B", "d2b3A", "d2b3A/1", "h21", "a35/2", "a35/1", "d2b3B/1", "n22", "a35/3",
    "h22.0", "h22.1", "d2aendB", "d2aendA", "p21a", "h22", "p22a", "q1a2", "q1a2/1", "a36", "p20a", "q2a2", "q2a2/1",
    "d2b4B", "d2b4B/1", "d2b4A", "d2b4A/1", "n23", "q0a2", "q0a2/1", "h23.0", "q1a3", "q1a3/1", "h23.1", "h23",
    "q2a3", "q2a3/1", "p23a", "q0a3", "q0a3/1", "d2bendB", "d2bendA", "p20b", "p21b", "q3a2", "q3a2/1", "p23b",
    "q0b2", "q0b2/1", "q1b2", "q1b2/1", "p22b", "q3b2", "q3b2/1", "q3a3", "q3a3/1", "q2b2", "q0b3", "q2b2/1", "q1b3",
    "q0b3/1", "q1b3/1", "q3b3", "q3a4", "q3b3/1", "q2a4", "q2b3", "q0a4", "q2b3/1", "q0b4", "q1a4", "q1b4", "q3b4",
    "q2b4",
)


class Task:
    def __init__(self, name, waits=(), after=(), work=None, cost=0.05, sends=(), rank=0):
        self.name, self.waits, self.after = name, list(waits), list(after)
        self.work, self.cost, self.sends, self.rank = work, cost, list(sends), rank


def arranged(tasks):
    named = {task.name: task for task in tasks}
    steps = []
    for entry in ORDER:
        name, _, number = entry.partition("/")
        steps.append((named[name], int(number or 0)))
    wanted = sum(max(1, len(task.sends)) for task in tasks)
    assert len(set(ORDER)) == len(ORDER) == wanted, (len(ORDER), wanted)
    return steps


def build(ring, fs, tp, refs, enter):
    (
        tokens, first_gain, first_gate, first_up, first_down, mix_gain, mix_input, pool_weight, pool_scale, mix_output,
        second_gain, second_gate, second_up, second_down, out,
        gains, pool_w, scales, gates, ups, downs, mixw, feats, middle, hidden, normed, run_normed, first_run, pool_in, halo, mapped_run,
        rows_part, rows_sib, rows_half, rows_full, cols_part, cols_sib, cols_half, cols_full,
        bank,
    ) = refs
    z, y = lax.div(fs, ring), lax.rem(fs, ring)
    x, c = lax.div(tp, 2), lax.rem(tp, 2)
    other = 1 - c
    blocks = 2 * ring
    rows_all, width = tokens.shape
    model = blocks * width
    length = rows_all // CHUNKS
    run = length // blocks
    lane = 128
    units = hidden.shape[1]

    def step(value, by):
        return lax.rem(value + by + ring, ring)

    devices = {
        "y+": {"fs": z * ring + step(y, 1)}, "y-": {"fs": z * ring + step(y, -1)},
        "z+": {"fs": step(z, 1) * ring + y}, "z-": {"fs": step(z, -1) * ring + y},
        "x+": {"tp": step(x, 1) * 2 + c}, "x-": {"tp": step(x, -1) * 2 + c},
        "c": {"tp": x * 2 + other},
        "ypair": {"fs": z * ring + y + 1 - 2 * lax.rem(y, 2)},
        "zpair": {"fs": (z + 1 - 2 * lax.rem(z, 2)) * ring + y},
        "next": {"tp": lax.rem(tp + 1, blocks)}, "last": {"tp": lax.rem(tp + blocks - 1, blocks)},
    }
    tasks = []

    def add(*args, **kwargs):
        tasks.append(Task(*args, **kwargs))

    def size_of(shape):
        total = 2
        for extent in shape:
            total *= extent
        return total

    def remote(event, link, make_src, make_dst, shape):
        def make(send_slot, recv_slot):
            return pltpu.make_async_remote_copy(
                src_ref=make_src(), dst_ref=make_dst(), send_sem=bank.at[send_slot], recv_sem=bank.at[recv_slot],
                device_id=devices[link], device_id_type=MESH,
            )

        return (event, {"next": "x+", "ypair": "y+", "zpair": "z+"}.get(link, link), size_of(shape), make)

    def same(event, link, make_ref, shape):
        return remote(event, link, make_ref, make_ref, shape)

    def local(event, make_src, make_dst, shape):
        return (event, "l", size_of(shape), lambda slot: pltpu.make_async_copy(make_src(), make_dst(), bank.at[slot]))

    def gather_weights(name, buf, loaded, before):
        rows, cols = buf.shape[2], buf.shape[3]
        half, quarter = rows // 2, rows // 4

        def phases(letter, near, far, begin, at, line):
            low, high = (begin, quarter), (begin + quarter, quarter)
            whole = (begin, half)
            tag = f"{name}{letter}"

            def block(event, link, d, e, part):
                return same(f"{tag}{event}", link, lambda: at(d, e, part), (part[1], cols))

            def both(event, d, e, part=whole):
                return [block(event + sign, far + sign, d, e, part) for sign in "+-"]

            first = [block("1" + sign, near + sign, 0, 0, whole) for sign in "+-"]
            if name in FINE:
                first += both("3o", 0, 0)
                second = both("3n", -1, 0) + both("3m", 1, 0)
                third = both("3f", 2, 0)
            else:
                second = []
                third = [same(f"{tag}3{sign}", far + sign, lambda: line(0, whole), (ring, half, cols)) for sign in "+-"]
            add(f"{name}2{letter}", waits=[f"{tag}1+", f"{tag}1-"], sends=[
                block("2+", near + "+", -1, 0, low), block("2-", near + "-", 1, 0, high),
            ] + second)
            add(f"{name}3{letter}", waits=[f"{tag}2+", f"{tag}2-"], after=[f"{name}2{letter}"], sends=third)
            if name in FINE:
                for which, spots in (("o", (0,)), ("n", (-1, 1)), ("f", (2,))):
                    arrivals = [f"{tag}3{w}{sign}" for w in {"o": "o", "n": "nm", "f": "f"}[which] for sign in "+-"]
                    sends = []
                    for d in spots:
                        sends += [
                            block(f"4{which}{d}+", far + "+", d, -1, low), block(f"4{which}{d}-", far + "-", d, 1, high),
                        ]
                    add(f"{name}4{letter}{which}", waits=arrivals, sends=sends)
                add(f"{name}4{letter}", after=[f"{name}4{letter}{w}" for w in "onf"], cost=0.0)
                last = [f"{tag}4{w}{d}{sign}" for w, d in (("o", 0), ("n", -1), ("n", 1), ("f", 2)) for sign in "+-"]
            else:
                add(f"{name}4{letter}", waits=[f"{tag}3+", f"{tag}3-"], sends=[
                    same(f"{tag}4+", far + "+", lambda: line(-1, low), (ring, quarter, cols)),
                    same(f"{tag}4-", far + "-", lambda: line(1, high), (ring, quarter, cols)),
                ])
                last = [f"{tag}4+", f"{tag}4-"]
            add(f"{name}end{letter}", waits=last, cost=0.02, after=[f"{name}4{letter}"])
            return first

        first = phases(
            "A", "y", "z", 0, lambda d, e, part: buf.at[step(z, e), step(y, d), pl.ds(*part)],
            lambda e, part: buf.at[step(z, e), :, pl.ds(*part)],
        ) + phases(
            "B", "z", "y", half, lambda d, e, part: buf.at[step(z, d), step(y, e), pl.ds(*part)],
            lambda e, part: buf.at[:, step(y, e), pl.ds(*part)],
        )
        add(f"{name}1", waits=loaded, after=before, sends=first)

    def ends(*names):
        return [f"{name}end{half}" for name in names for half in "AB"]

    def block_of(xx, cc):
        return xx * 2 + cc

    def send_own(tag, view, size):
        def own():
            return view(tp, 2)
        return [
            same(f"{tag}p", "x+", own, (size,)), same(f"{tag}m", "x-", own, (size,)), same(f"{tag}s0", "c", own, (size,)),
        ]

    def gather_blocks(tag, view, size):
        def at(by, part):
            return view(block_of(step(x, by), c), part)

        add(f"{tag}5", waits=[f"{tag}p", f"{tag}m"], sends=[
            same(f"{tag}fp", "x+", lambda: at(-1, 0), (size // 2,)),
            same(f"{tag}fm", "x-", lambda: at(1, 1), (size // 2,)),
            same(f"{tag}s1", "c", lambda: at(-1, 2), (size,)),
            same(f"{tag}s2", "c", lambda: at(1, 2), (size,)),
        ])
        add(f"{tag}6", waits=[f"{tag}fp", f"{tag}fm"], after=[f"{tag}5"], sends=[
            same(f"{tag}s3", "c", lambda: at(2, 2), (size,)),
        ])
        return dict(waits=[f"{tag}s{n}" for n in range(4)], after=[f"{tag}6"])

    def scatter_sums(tag, bufs, start, extent, before, finish):
        part, sib, half_recv, full_recv = bufs
        cols = part.shape[3]
        rows, half = pl.ds(start, extent), extent // 2
        low, high, compact = pl.ds(start, half), pl.ds(start + half, half), pl.ds(start // 2, half)
        far, right, left = step(x, 2), step(x, 1), step(x, -1)

        def pair(target, which):
            return part[target, c, which].astype(F32) + sib[target, which].astype(F32)

        def fold_far():
            part[far, c, rows] = pair(far, rows).astype(BF16)

        add(f"{tag}2", waits=[f"{tag}sib"], after=before, work=fold_far, cost=0.05, sends=[
            remote(f"{tag}hp", "x+", lambda: part.at[far, c, low], lambda: half_recv.at[0, compact], (half, cols)),
            remote(f"{tag}hm", "x-", lambda: part.at[far, c, high], lambda: half_recv.at[1, compact], (half, cols)),
        ])

        def fold_near():
            for target, extra, plain, number in ((right, low, high, 0), (left, high, low, 1)):
                part[target, c, extra] = (pair(target, extra) + half_recv[number, compact].astype(F32)).astype(BF16)
                part[target, c, plain] = pair(target, plain).astype(BF16)

        add(f"{tag}3", waits=[f"{tag}hp", f"{tag}hm"], after=[f"{tag}2"], work=fold_near, cost=0.05, sends=[
            remote(f"{tag}dp", "x+", lambda: part.at[right, c, rows], lambda: full_recv.at[0, rows], (extent, cols)),
            remote(f"{tag}dm", "x-", lambda: part.at[left, c, rows], lambda: full_recv.at[1, rows], (extent, cols)),
        ])

        def total(span):
            return (
                part[x, c, rows, span].astype(F32) + sib[x, rows, span].astype(F32)
                + full_recv[0, rows, span].astype(F32) + full_recv[1, rows, span].astype(F32)
            )

        work, sends, cost = finish(total)
        add(f"{tag}4", waits=[f"{tag}dp", f"{tag}dm"], after=[f"{tag}3"], work=work, cost=cost, sends=sends)

    def send_parts(tag, bufs, start, extent):
        part, sib = bufs[:2]
        rows = pl.ds(start, extent)
        return [remote(
            f"{tag}sib", "c", lambda: part.at[:, other, rows], lambda: sib.at[:, rows], (ring, extent, part.shape[3]),
        )]

    sub = 16

    def scaled(values, gains):
        squares = functools.reduce(lambda a, b: a + b, [v * v for v in values])
        mean = jnp.sum(squares, axis=-1, keepdims=True) * (1.0 / model)
        factor = lax.rsqrt(mean + EPSILON)
        return [(v * factor * g).astype(BF16) for v, g in zip(values, gains)]

    def normalize_rows(read, gain, start):
        def body(i, carry):
            base = pl.multiple_of(start + i * sub, sub)
            factors = [gains[gain, :, b * width:(b + 1) * width] for b in range(blocks)]
            for b, v in enumerate(scaled([read(b, pl.ds(base, sub)).astype(F32) for b in range(blocks)], factors)):
                normed[pl.ds(base, sub), b * width:(b + 1) * width] = v
            return carry

        lax.fori_loop(0, length // sub, body, 0, unroll=2)

    tile = 256

    def hidden_rows(which, start, n):
        def work():
            cols = slice(n * tile, (n + 1) * tile)
            gate_w = gates[which, :, :, :, cols].reshape(model, tile)
            up_w = ups[which, :, :, :, cols].reshape(model, tile)
            both = jnp.dot(
                normed[pl.ds(start, length), :], jnp.concatenate([gate_w, up_w], axis=1), preferred_element_type=F32
            )
            gated, upward = both[:, :tile], both[:, tile:]
            value = gated / (1.0 + jnp.exp(-gated)) * upward
            hidden[pl.ds(start, length), cols] = value.astype(BF16)
        return work

    def add_hidden(name, which, start, behind, rank):
        count = units // tile
        for n in range(count):
            last = n == count - 1
            add(name if last else f"{name}.{n}", after=behind, work=hidden_rows(which, start, n), cost=0.72, rank=rank)
            behind = [f"{name}.{n}"]

    def down_rows(which, part, start, store):
        def work():
            def body(n, carry):
                columns = []
                for i in range(ring):
                    if which:
                        column = downs[which, part, n * 2 + i // 2, i % 2 * 2:i % 2 * 2 + 2]
                    else:
                        column = downs[which, part, pl.ds(n * 2, 2), i]
                    columns.append(column.reshape(units, lane))
                value = jnp.dot(
                    hidden[pl.ds(start, length), :], jnp.concatenate(columns, axis=1), preferred_element_type=F32
                )
                store(n, value.astype(BF16))
                return carry

            lax.fori_loop(0, ring // 2, body, 0)
        return work

    wide = ring * lane

    def first_finish(k, part):
        start = k * length

        def finish(total):
            def work():
                place = pl.ds(pl.multiple_of(start + tp * run, run), run)
                for packed in range(ring):
                    b = (packed // 2 * 2 + part) * 2 + packed % 2
                    value = feats[b, place, :].astype(F32) + 0.5 * total(slice(packed * width, (packed + 1) * width))
                    first_run[k * run:(k + 1) * run, b * width:(b + 1) * width] = value.astype(BF16)
            return work, [], 0.05
        return finish

    def pool_in_rows(k):
        def work():
            factors = [gains[1, :, b * width:(b + 1) * width] for b in range(blocks)]
            for base in range(0, run, sub):
                rows = pl.ds(k * run + base, sub)
                spans = [slice(b * width, (b + 1) * width) for b in range(blocks)]
                for span, v in zip(spans, scaled([first_run[rows, span].astype(F32) for span in spans], factors)):
                    run_normed[base:base + sub, span] = v

            def body(n, carry):
                columns = [mixw[n * ring + i, :, :, 0:lane, :].reshape(model, lane) for i in range(ring)]
                value = jnp.dot(run_normed[...], jnp.concatenate(columns, axis=1), preferred_element_type=F32)
                pool_in[k, :, pl.ds(pl.multiple_of(n * wide, wide), wide)] = value.astype(BF16)
                return carry

            lax.fori_loop(0, blocks // ring, body, 0)
            if k == 0:
                halo[0] = jnp.zeros(halo.shape[1:], BF16)
        return work

    def mixer_rows(k):
        start = k * length

        def work():
            position = start + tp * run + lax.broadcasted_iota(jnp.int32, (run, lane), 0)
            slot = k + jnp.minimum(tp, 1)
            for b in range(blocks):
                span = slice(b * lane, (b + 1) * lane)
                window = 2 << (b % 4)
                current = pool_in[k, :, span].astype(F32)
                total = jnp.concatenate([halo[slot, :, span].astype(F32), current], axis=0)
                shift = 1
                while shift < window:
                    total = total + pltpu.roll(total, shift, 0)
                    shift *= 2
                number = jnp.minimum(position + 1, window).astype(F32)
                pooled = (total[HALO:, :] / number - current).astype(BF16)
                mapped = jnp.dot(pooled, pool_w[b], preferred_element_type=F32)
                mapped_run[:, span] = (mapped * scales[b:b + 1, :]).astype(BF16)
        return work

    def mixer_out(k):
        start = k * length

        def work():
            place = pl.ds(pl.multiple_of(start + tp * run, run), run)

            def body(n, carry):
                columns = [mixw[:, n, i, lane:2 * lane, :].reshape(blocks * lane, lane) for i in range(ring)]
                value = jnp.dot(mapped_run[...], jnp.concatenate(columns, axis=1), preferred_element_type=F32)
                cols = pl.ds(pl.multiple_of(n * wide, wide), wide)
                value = first_run[k * run:(k + 1) * run, cols].astype(F32) + value
                middle[place, cols] = value.astype(BF16)
                return carry

            lax.fori_loop(0, ring, body, 0)
        return work

    token_load = local("tok", lambda: tokens, lambda: feats.at[0 + tp], (rows_all, width))
    add("tokload", sends=[token_load], cost=0.01, rank=-3)
    items = {
        "g1": (gates.at[0], [(first_gate, 0, lane)]), "u1": (ups.at[0], [(first_up, 0, lane)]),
        "mx": (mixw.at[tp], [(mix_input, 0, lane), (mix_output, lane, lane)]),
        "g2": (gates.at[1], [(second_gate, 0, lane)]), "u2": (ups.at[1], [(second_up, 0, lane)]),
    }
    share = units // 2
    for number, (name, source, place) in enumerate((("d1", first_down, z), ("d2", second_down, y))):
        parity = lax.rem(place, 2)
        partner = place + 1 - 2 * parity
        kept = pl.ds(pl.multiple_of(parity * share, share), share)
        given = pl.ds(pl.multiple_of((1 - parity) * share, share), share)
        there = (z, partner) if number else (partner, y)
        add(f"{name}load", cost=0.01, rank=-2, sends=[local(
            f"{name}l", lambda source=source, kept=kept: source.at[kept],
            lambda number=number, parity=parity: downs.at[number, parity, z, y], (share, lane),
        )])
        add(f"{name}pair", after=["entered"], cost=0.05, rank=1, sends=[remote(
            f"{name}p", ("zpair", "ypair")[number], lambda source=source, given=given: source.at[given],
            lambda number=number, there=there, parity=parity: downs.at[number, parity, there[0], there[1]], (share, lane),
        )])
        add(f"{name}ready", waits=[f"{name}l", f"{name}p"], cost=0.01, rank=0)
        for part, letter in enumerate("ab"):
            items[name + letter] = (downs.at[number, part], None)
    for name, (buf, pieces) in items.items():
        before = ["entered"]
        events = []
        if pieces is None:
            before.append(f"{name[:2]}ready")
        else:
            loads = [
                local(
                    f"{name}l{number}", lambda src=src: src,
                    lambda buf=buf, start=start, extent=extent: buf.at[z, y, pl.ds(start, extent)], (extent, buf.shape[3]),
                )
                for number, (src, start, extent) in enumerate(pieces)
            ]
            add(f"{name}load", sends=loads, cost=0.01, rank=-2)
            events = [e[0] for e in loads]
        gather_weights(name, buf, events, before)
    small = [
        (f"small{n}", src, dst) for n, (src, dst) in enumerate((
            (first_gain, gains.at[0]), (mix_gain, gains.at[1]), (second_gain, gains.at[2]), (pool_weight, pool_w),
            (pool_scale, scales),
        ))
    ]
    add("smallload", cost=0.01, rank=-1, sends=[
        local(event, lambda src=src: src, lambda dst=dst: dst, (8, 2048)) for event, src, dst in small
    ])
    add("entered", cost=3.0, rank=-1, after=["tokload", "smallload", "d1load", "d2load"] + [f"{n}load" for n in ("g1", "u1", "mx", "g2", "u2")],
        work=enter)

    def token_view(block, part):
        half = rows_all // 2
        return feats.at[block, pl.ds(*((0, half), (half, half), (0, rows_all))[part])]

    add("tok1", waits=["tok"], after=["entered"], sends=send_own("t", token_view, rows_all * width))
    add("smallend", waits=[event for event, _, _ in small], after=["entered"], cost=0.01)
    add("tokend", cost=0.01, **gather_blocks("t", token_view, rows_all * width))
    for tag, begin, half_name in (("xi", 0, "A"), ("xo", lane, "B")):
        def mix_view(block, part, begin=begin):
            half = ring // 2
            return mixw.at[block, pl.ds(*((0, half), (half, half), (0, ring))[part]), :, pl.ds(begin, lane)]

        size = ring * ring * lane * lane
        add(f"{tag}1", after=[f"mxend{half_name}"], sends=send_own(tag, mix_view, size))
        add(f"{tag}end", cost=0.01, **gather_blocks(tag, mix_view, size))

    by_rows = [tuple(ref.at[part] for ref in (rows_part, rows_sib, rows_half, rows_full)) for part in range(2)]
    by_cols = [tuple(ref.at[part] for ref in (cols_part, cols_sib, cols_half, cols_full)) for part in range(2)]
    for k in range(CHUNKS):
        start = k * length
        rows = pl.ds(start, length)
        before = [f"m{k - 1}"] if k else []
        add(f"n1{k}", after=["tokend", "smallend"], cost=0.8, rank=3,
            work=functools.partial(normalize_rows, lambda b, place: feats[b, place, :], 0, start))
        add_hidden(f"h1{k}", 0, start, [f"n1{k}"] + ends("g1", "u1"), 2)

        for part, letter in enumerate("ab"):
            def store_rows(n, value, k=k, part=part):
                cols = pl.ds(pl.multiple_of(n * wide, wide), wide)
                for b in range(blocks):
                    rows_part[part, b // 2, b % 2, k * run:(k + 1) * run, cols] = value[b * run:(b + 1) * run, :]

            add(f"p1{k}{letter}", after=[f"h1{k}"] + ends(f"d1{letter}"), work=down_rows(0, part, start, store_rows),
                cost=0.7, rank=1, sends=send_parts(f"r{k}{letter}", by_rows[part], k * run, run))
            scatter_sums(f"r{k}{letter}", by_rows[part], k * run, run, [f"p1{k}{letter}"], first_finish(k, part))
        add(f"i{k}", after=[f"r{k}a4", f"r{k}b4", "xiend"], work=pool_in_rows(k), cost=1.0, rank=1, sends=[remote(
            f"halo{k}", "next", lambda k=k: pool_in.at[k, pl.ds(run - HALO, HALO)], lambda k=k: halo.at[k + 1],
            (HALO, blocks * lane),
        )])

        def run_view(block, part, start=start):
            half = run // 2
            begin, extent = ((0, half), (half, half), (0, run))[part]
            return middle.at[pl.ds(pl.multiple_of(start + block * run + begin, half), extent)]

        add(f"b{k}", waits=[f"halo{k}"], after=[f"i{k}"] + before, work=mixer_rows(k), cost=0.6, rank=1)
        add(f"m{k}", after=[f"b{k}", "xoend"], work=mixer_out(k), cost=0.75, rank=1,
            sends=send_own(f"a{k}", run_view, run * model))
        seen = gather_blocks(f"a{k}", run_view, run * model)
        add(f"n2{k}", waits=seen["waits"], after=seen["after"] + [f"h1{k}"], cost=0.8, rank=2,
            work=functools.partial(
                normalize_rows, lambda b, place: middle[place, b * width:(b + 1) * width], 2, start))
        add_hidden(f"h2{k}", 1, start, [f"n2{k}", f"p1{k}a", f"p1{k}b"] + ends("g2", "u2"), 2)

        for part, letter in enumerate("ab"):
            def store_cols(n, value, rows=rows, part=part):
                for i in range(ring):
                    cols_part[part, n * 2 + i // 2, i % 2, rows] = value[:, i * lane:(i + 1) * lane]

            add(f"p2{k}{letter}", after=[f"h2{k}"] + ends(f"d2{letter}"), work=down_rows(1, part, start, store_cols),
                cost=0.75, rank=1, sends=send_parts(f"q{k}{letter}", by_cols[part], start, length))

            def last_finish(total, rows=rows, part=part):
                def work():
                    cols = pl.ds(pl.multiple_of(tp * width + part * lane, lane), lane)
                    value = middle[rows, cols].astype(F32) + 0.5 * total(slice(None))
                    out[rows, part * lane:(part + 1) * lane] = value.astype(BF16)
                return work, [], 0.1

            scatter_sums(f"q{k}{letter}", by_cols[part], start, length, [f"p2{k}{letter}"], last_finish)
    return tasks, devices

def layer_kernel(ring, *refs):
    fs, tp = lax.axis_index("fs"), lax.axis_index("tp")
    places = {}

    def enter():
        devices = places["devices"]
        barrier = pltpu.get_barrier_semaphore()
        greeted = [device for link, device in devices.items() if "pair" not in link]
        for device in greeted:
            pl.semaphore_signal(barrier, inc=1, device_id=device, device_id_type=MESH)
        pl.semaphore_wait(barrier, len(greeted))

    tasks, places["devices"] = build(ring, fs, tp, refs, enter)
    run_steps(tasks, arranged(tasks), refs[-1], *[refs[n] for n in MEASURES])


def run_steps(tasks, steps, bank, small, large):
    used = [0]

    def new_slot():
        used[0] += 1
        return used[0] - 1

    def sized(size, slot):
        unit = large.shape[1] * 2
        if size % (8 * unit) == 0:
            ref = large.at[pl.ds(0, size // unit)]
        else:
            unit = small.shape[2] * 2
            assert size % (8 * unit) == 0 and size // unit <= small.shape[1], size
            ref = small.at[0, pl.ds(0, size // unit)]
        return pltpu.make_async_copy(ref, ref, bank.at[slot])

    slots, sizes = {}, {}
    for task in tasks:
        for event, link, size, _ in task.sends:
            sizes[event] = (link, size)
    for task in tasks:
        links = {sizes[event][0] == "l" for event in task.waits}
        for local in links:
            slot = new_slot()
            for event in task.waits:
                if (sizes[event][0] == "l") == local:
                    slots[event] = new_slot() if local else slot
    bounds = (small.shape[1] * small.shape[2] * 2, large.shape[0] * large.shape[1] * 2)
    groups, sent, copies, waited = {}, [], {}, set()
    for task, number in steps:
        if number == 0:
            remote_bytes = 0
            for event in task.waits:
                if sizes[event][0] == "l":
                    copies[event].wait()
                else:
                    assert event in copies, event
                    remote_bytes += sizes[event][1]
                    slot = slots[event]
                waited.add(event)
            if remote_bytes:
                sized(remote_bytes, slot).wait()
            if task.work is not None:
                task.work()
        for event, link, size, make in task.sends[number:number + 1]:
            if link == "l":
                copy = make(slots[event])
            else:
                kind = int(size % (16 * large.shape[1]) == 0)
                if kind not in groups or groups[kind][0] + size > bounds[kind]:
                    groups[kind] = [0, new_slot()]
                    sent.append(groups[kind])
                groups[kind][0] += size
                copy = make(groups[kind][1], slots[event])
            copy.start()
            copies[event] = copy
    assert waited == set(sizes)
    for total, slot in sent:
        sized(total, slot).wait()
    assert used[0] == bank.shape[0], used


def scratch_of(ring, rows, width, units):
    blocks, run, lane = 2 * ring, rows // CHUNKS // (2 * ring), 128
    model, runs = blocks * width, rows // (2 * ring)
    return [
        pltpu.VMEM((3, 1, model), F32),
        pltpu.VMEM((blocks, lane, lane), BF16),
        pltpu.VMEM((blocks, lane), F32),
        pltpu.VMEM((2, ring, ring, lane, units), BF16),
        pltpu.VMEM((2, ring, ring, lane, units), BF16),
        pltpu.VMEM((2, 2, ring, ring, units // 2, lane), BF16),
        pltpu.VMEM((blocks, ring, ring, 2 * lane, lane), BF16),
        pltpu.VMEM((blocks, rows, width), BF16),
        pltpu.VMEM((rows, model), BF16),
        pltpu.VMEM((rows, units), BF16),
        pltpu.VMEM((rows, model), BF16),
        pltpu.VMEM((run, model), BF16),
        pltpu.VMEM((runs, model), BF16),
        pltpu.VMEM((CHUNKS, run, blocks * lane), BF16),
        pltpu.VMEM((CHUNKS + 1, HALO, blocks * lane), BF16),
        pltpu.VMEM((run, blocks * lane), BF16),
        pltpu.VMEM((2, ring, 2, runs, model // 2), BF16),
        pltpu.VMEM((2, ring, runs, model // 2), BF16),
        pltpu.VMEM((2, 2, runs // 2, model // 2), BF16),
        pltpu.VMEM((2, 2, runs, model // 2), BF16),
        pltpu.VMEM((2, ring, 2, rows, width // 2), BF16),
        pltpu.VMEM((2, ring, rows, width // 2), BF16),
        pltpu.VMEM((2, 2, rows // 2, width // 2), BF16),
        pltpu.VMEM((2, 2, rows, width // 2), BF16),
        pltpu.SemaphoreType.DMA((SEMAPHORES,)),
    ]


def per_device(
    tokens, first_gain, first_gate, first_up, first_down, mix_gain, mix_input, pool_weight, pool_scale, mix_output,
    second_gain, second_gate, second_up, second_down, *, ring,
):
    rows, width = tokens.shape
    anywhere = pl.BlockSpec(memory_space=pl.ANY)
    inside = pl.BlockSpec(memory_space=pltpu.VMEM)
    return pl.pallas_call(
        functools.partial(layer_kernel, ring),
        out_shape=pltpu.VMEM((rows, width), BF16),
        in_specs=[anywhere] * 14,
        out_specs=inside,
        scratch_shapes=scratch_of(ring, rows, width, first_gate.shape[1]),
        compiler_params=pltpu.CompilerParams(collective_id=0, has_side_effects=True, vmem_limit_bytes=VMEM_LIMIT),
    )(
        tokens, first_gain.reshape(1, -1), first_gate, first_up, first_down, mix_gain.reshape(1, -1), mix_input,
        pool_weight, pool_scale.reshape(-1, 128), mix_output, second_gain.reshape(1, -1), second_gate, second_up,
        second_down,
    )


def solution(mesh):
    weight, turned = P("fs", "tp"), P("tp", "fs")
    return jax.shard_map(
        functools.partial(per_device, ring=mesh.shape["tp"] // 2),
        mesh=mesh,
        in_specs=(
            P("fs", "tp"), P(), weight, weight, turned, P(), weight, P(), P(), turned, P(), weight, weight, turned,
        ),
        out_specs=P("fs", "tp"),
        check_vma=False,
    )
```
